256 devices in a mesh: fs: 32 (over z, y), tp: 8 (over x, core).
Axes of the slice: x: 4, y: 4, z: 8, core: 2. Of those that a mesh axis runs over, the one named last changes fastest.
Arguments:
- tokens: bfloat16 [32768, 2048], P(('fs', 'tp')), may hold values from -6 to 6
- norm_one: float32 [2048], replicated, may hold values from 0.1 to 1.9
- gate_one: bfloat16 [2048, 4608], P('fs', 'tp'), may hold values from -0.125 to 0.125
- up_one: bfloat16 [2048, 4608], P('fs', 'tp'), may hold values from -0.125 to 0.125
- down_one: bfloat16 [4608, 2048], P('tp', 'fs'), may hold values from -0.1875 to 0.1875
- norm_two: float32 [2048], replicated, may hold values from 0.1 to 1.9
- gate_two: bfloat16 [2048, 4608], P('fs', 'tp'), may hold values from -0.125 to 0.125
- up_two: bfloat16 [2048, 4608], P('fs', 'tp'), may hold values from -0.125 to 0.125
- down_two: bfloat16 [4608, 2048], P('tp', 'fs'), may hold values from -0.1875 to 0.1875
Outputs:
- result: bfloat16 [32768, 2048], P(('fs', 'tp'))
The draws below stay inside these ranges and needn't reach their ends.
All inputs are finite; a program needn't handle non-finite values.
Results may differ from the reference program's by a relative error of at most 0.015.
Values may be sent and summed in bfloat16 or wider, within the bound.
A program may use at most 64 MiB of HBM per device.

```python
import jax
import jax.numpy as jnp
from jax import lax

D = 2048
FF = 4608
TOKENS = 32768
N_FS = 32
N_TP = 8


def block_scale(stream_key, dims, pieces, least, largest):
    factor_of = 1.0
    for axis_at, parts in pieces:
        steps = jax.random.uniform(jax.random.fold_in(jax.random.fold_in(stream_key, 6), axis_at), (parts,), jnp.float32, least / len(pieces), largest / len(pieces))
        factor_of = factor_of * jnp.repeat(jnp.exp(steps), dims[axis_at] // parts).reshape((-1,) + (1,) * (len(dims) - 1 - axis_at))
    return factor_of


def bell_draw(own_key, dims, scale, bound, split=(), dtype=jnp.bfloat16):
    level = block_scale(own_key, dims, split, -0.22, 0.18) if split else 1.0
    drawn = jax.random.normal(own_key, dims, jnp.float32) * scale * level
    return jnp.minimum(jnp.maximum(drawn, -bound), bound).astype(dtype)


def setup_inputs(seed: int = 0) -> dict:
    key_list = jax.random.split(jax.random.key(seed), 10)
    return {
        "tokens": bell_draw(key_list[0], (TOKENS, D), 1.0, 6.0, ((0, 256),)),
        "norm_one": jnp.clip(1.0 + 0.18 * jax.random.normal(key_list[1], (D,), jnp.float32), 0.1, 1.9),
        "gate_one": bell_draw(key_list[2], (D, FF), D ** -0.5, 0.125, ((0, 32), (1, 8))),
        "up_one": bell_draw(key_list[3], (D, FF), D ** -0.5, 0.125, ((0, 32), (1, 8))),
        "down_one": bell_draw(key_list[4], (FF, D), (FF // 4) ** -0.5, 0.1875, ((0, 8), (1, 32))),
        "norm_two": jnp.clip(1.0 + 0.18 * jax.random.normal(key_list[5], (D,), jnp.float32), 0.1, 1.9),
        "gate_two": bell_draw(key_list[6], (D, FF), D ** -0.5, 0.125, ((0, 32), (1, 8))),
        "up_two": bell_draw(key_list[7], (D, FF), D ** -0.5, 0.125, ((0, 32), (1, 8))),
        "down_two": bell_draw(key_list[8], (FF, D), (FF // 4) ** -0.5, 0.1875, ((0, 8), (1, 32))),
    }


eps = 1e-06

def normalize(rows, gain):
    values = rows.astype(jnp.float32)
    scaled = values * lax.rsqrt(lax.optimization_barrier(jnp.mean(values * values, axis=-1, keepdims=True)) + eps)
    return (scaled * gain.astype(jnp.float32)).astype(jnp.bfloat16)

def product(left, right):
    return jnp.dot(left.astype(jnp.float32), right.astype(jnp.float32), preferred_element_type=jnp.float32)

def half_step(rows, gain, gate_w, up_w, down_w):
    normed = normalize(rows, gain)
    hidden = (jax.nn.silu(product(normed, gate_w)) * product(normed, up_w)).astype(jnp.bfloat16)
    width = down_w.shape[0] // N_TP
    total = jnp.zeros((rows.shape[0], down_w.shape[1]), jnp.float32)
    for block in range(N_TP):
        partial_value = product(hidden[:, block * width:(block + 1) * width], down_w[block * width:(block + 1) * width])
        rounded = lax.optimization_barrier(partial_value.astype(jnp.bfloat16))
        total = total + rounded.astype(jnp.float32)
    return (rows.astype(jnp.float32) + 0.5 * total).astype(jnp.bfloat16)

def reference(tokens, norm_one, gate_one, up_one, down_one, norm_two, gate_two, up_two, down_two):

    def group_step(rows):
        middle = half_step(rows, norm_one, gate_one, up_one, down_one)
        return half_step(middle, norm_two, gate_two, up_two, down_two)
    grouped = tokens.reshape(N_FS, tokens.shape[0] // N_FS, tokens.shape[1])
    return lax.map(group_step, grouped).reshape(tokens.shape)
```

```python
import functools

import jax
import jax.numpy as jnp
from jax import lax
from jax.experimental import pallas as pl
from jax.experimental.pallas import tpu as pltpu
from jax.sharding import PartitionSpec as P

MESH = pl.DeviceIdType.MESH
EPS = 1e-06
NZ, NY, NX = 8, 4, 4
ROWS, D = 128, 2048
GU, DK, H = 1152, 640, 576
CH = 512
SEMS = 240


class Net:
    def __init__(self, send_sems, recv_sems):
        self.send_sems, self.recv_sems = send_sems, recv_sems
        self.index, self.sent = {}, []

    def slot(self, key):
        return self.index.setdefault(key, len(self.index))

    def send(self, key, src, dst, device):
        k = self.slot(key)
        copy = pltpu.make_async_remote_copy(
            src_ref=src,
            dst_ref=dst,
            send_sem=self.send_sems.at[k],
            recv_sem=self.recv_sems.at[k],
            device_id=device,
            device_id_type=MESH,
        )
        copy.start()
        self.sent.append(copy)

    def recv(self, key, ref, device):
        k = self.slot(key)
        pltpu.make_async_remote_copy(
            src_ref=ref,
            dst_ref=ref,
            send_sem=self.send_sems.at[k],
            recv_sem=self.recv_sems.at[k],
            device_id=device,
            device_id_type=MESH,
        ).wait_recv()

    def finish(self):
        for copy in self.sent:
            copy.wait_send()


def kernel(
    x_in, gu1_in, d1_in, gu2_in, d2_in, gain1, gain2, out_ref,
    xown, mid, wg1, wg2, wd1, wd2, xn1, xn2, acc, hid, keep,
    sb, rb, u1, u2, r1, r2, local_sems, send_sems, recv_sems,
):
    fs, tp = lax.axis_index("fs"), lax.axis_index("tp")
    z, y = lax.div(fs, NY), lax.rem(fs, NY)
    x, c = lax.div(tp, 2), lax.rem(tp, 2)
    oc = 1 - c

    def zz(k):
        return lax.rem(z + k + NZ, NZ)

    def yy(k):
        return lax.rem(y + k + NY, NY)

    def xx(k):
        return lax.rem(x + k + NX, NX)

    zdev = {s: (zz(s) * NY + y, tp) for s in (1, -1)}
    ydev = {s: (z * NY + yy(s), tp) for s in (1, -1)}
    xdev = {s: (fs, xx(s) * 2 + c) for s in (1, -1)}
    sib = (fs, x * 2 + oc)
    net = Net(send_sems, recv_sems)

    local = [
        pltpu.make_async_copy(src, dst, local_sems.at[k])
        for k, (src, dst) in enumerate(
            [
                (gu1_in, wg1.at[y, z]),
                (d1_in, wd1.at[z, y]),
                (x_in, xown),
                (gu2_in, wg2.at[y, z]),
                (d2_in, wd2.at[z, y]),
            ]
        )
    ]
    for copy in local:
        copy.start()

    barrier = pltpu.get_barrier_semaphore()
    for dev in (*zdev.values(), *ydev.values(), *xdev.values(), sib):
        pl.semaphore_signal(barrier, inc=1, device_id=dev, device_id_type=MESH)
    pl.semaphore_wait(barrier, 7)

    class Weights:
        def __init__(self, n, wg, wd):
            self.n, self.wg, self.wd = n, wg, wd

        def origin(self, i):
            if i == 0:
                return 0, 0, z
            s, k = (1, (i + 1) // 2) if i % 2 else (-1, i // 2)
            return s, k, zz(-s * k)

        def b1_start(self):
            for s in (1, -1):
                ref = self.wg.at[y, z]
                net.send((self.n, "b1", s, 1), ref, ref, zdev[s])

        def acquire(self, i):
            s, k, o = self.origin(i)
            ref = self.wg.at[y, o]
            net.recv((self.n, "b1", s, k), ref, zdev[-s])
            if k < (4 if s == 1 else 3):
                net.send((self.n, "b1", s, k + 1), ref, ref, zdev[s])

        def h1(self, i):
            ref = self.wg.at[y, self.origin(i)[2]]
            for s in (1, -1):
                net.send((self.n, "h1", s, i), ref, ref, ydev[s])

        def piece(self, i):
            if i:
                self.acquire(i)
            self.h1(i)

        def h2(self, i):
            o = self.origin(i)[2]
            for s in (1, -1):
                ref = self.wg.at[yy(-s), o]
                net.recv((self.n, "h1", s, i), ref, ydev[-s])
                if (i % 2 == 0) == (s == 1):
                    net.send((self.n, "h2", i), ref, ref, ydev[s])

        def h2_wait(self, i):
            ref = self.wg.at[yy(2), self.origin(i)[2]]
            net.recv((self.n, "h2", i), ref, ydev[-1 if i % 2 == 0 else 1])

        def a1_start(self):
            ref = self.wd.at[z, y]
            for s in (1, -1):
                net.send((self.n, "a1", s), ref, ref, ydev[s])

        def a1_forward(self):
            ref = self.wd.at[z, yy(-1)]
            net.recv((self.n, "a1", 1), ref, ydev[-1])
            net.send((self.n, "a1f"), ref, ref, ydev[1])
            net.recv((self.n, "a1", -1), self.wd.at[z, yy(1)], ydev[1])

        def a2_start(self):
            net.recv((self.n, "a1f"), self.wd.at[z, yy(2)], ydev[-1])
            for q in (0, 1):
                ref = self.wd.at[z, pl.ds(2 * q, 2)]
                for s in (-1, 1):
                    net.send((self.n, "a2", s, q, 1), ref, ref, zdev[s])

        def a2_hop(self, k):
            for q in (0, 1):
                for s, last in ((-1, 4), (1, 3)):
                    if k <= last:
                        ref = self.wd.at[zz(-s * k), pl.ds(2 * q, 2)]
                        net.recv((self.n, "a2", s, q, k), ref, zdev[-s])
                        if k < last:
                            net.send((self.n, "a2", s, q, k + 1), ref, ref, zdev[s])

    w1, w2 = Weights(1, wg1, wd1), Weights(2, wg2, wd2)
    offsets = (0, -1, 1, 2)

    class Gather:
        def __init__(self, n, xn):
            self.n, self.xn = n, xn

        def put(self, src, gain):
            lane = lax.broadcasted_iota(jnp.int32, (32, 128), 1)

            @pl.loop(0, ROWS // 32)
            def _(b):
                rows = pl.ds(pl.multiple_of(b * 32, 32), 32)
                v = src[rows, :].astype(jnp.float32)
                mean = jnp.mean(v * v, axis=-1, keepdims=True)
                n = v * lax.rsqrt(mean + EPS) * gain[...]
                for j in range(4):
                    for i in range(4):
                        at = 512 * i + 128 * (j // 2)
                        one, two = n[:, at : at + 128], n[:, at + 256 : at + 384]
                        if j % 2 == 0:
                            tile = jnp.where(lane < 64, one, pltpu.roll(two, 64, 1))
                        else:
                            tile = jnp.where(lane < 64, pltpu.roll(one, 64, 1), two)
                        self.xn[j, c, x, rows, 128 * i : 128 * i + 128] = tile.astype(jnp.bfloat16)

        def g0(self, s):
            j = yy(offsets[s])
            ref = self.xn.at[j, c, x]
            for d in (1, -1):
                net.send((self.n, "g1", d, s), ref, ref, xdev[d])
            net.send((self.n, "gs", 0, s), ref, ref, sib)

        def g1(self, s):
            j = yy(offsets[s])
            for d in (1, -1):
                ref = self.xn.at[j, c, xx(-d)]
                net.recv((self.n, "g1", d, s), ref, xdev[-d])
                half = self.xn.at[j, c, xx(-d), pl.ds(0 if d == 1 else 64, 64)]
                net.send((self.n, "g2", d, s), half, half, xdev[d])
                net.send((self.n, "gs", d, s), ref, ref, sib)

        def g2(self, s):
            j = yy(offsets[s])
            for d in (1, -1):
                half = self.xn.at[j, c, xx(2), pl.ds(0 if d == 1 else 64, 64)]
                net.recv((self.n, "g2", d, s), half, xdev[-d])
            ref = self.xn.at[j, c, xx(2)]
            net.send((self.n, "gs", 2, s), ref, ref, sib)

        def g3(self, s):
            j = yy(offsets[s])
            for d, k in ((0, 0), (1, -1), (-1, 1), (2, 2)):
                net.recv((self.n, "gs", d, s), self.xn.at[j, oc, xx(k)], sib)

    def gate_up(xn, wg, s):
        j = yy(offsets[s])

        @pl.loop(0, 2)
        def _(i):
            rows = xn[j, i].reshape(4 * ROWS, CH)
            part = jnp.dot(rows, wg[j].reshape(CH, GU), preferred_element_type=jnp.float32)
            if s:
                acc[i] += part
            else:
                acc[i] = part

    def activate():
        lane = lax.broadcasted_iota(jnp.int32, (64, 128), 1)

        @pl.loop(0, 16)
        def _(b):
            i, rows = lax.div(b, 8), pl.ds(pl.multiple_of(lax.rem(b, 8) * 64, 64), 64)
            for n in range(4):
                g = acc[i, rows, 128 * n : 128 * n + 128]
                u = acc[i, rows, 512 + 128 * n : 640 + 128 * n]
                h = g / (1.0 + jnp.exp(-g)) * u
                hid[i, rows, 128 * n : 128 * n + 128] = h.astype(jnp.bfloat16)
            t = acc[i, rows, 1024:1152]
            h = t / (1.0 + jnp.exp(-t)) * pltpu.roll(t, 64, 1)
            hid[i, rows, 512:640] = jnp.where(lane < 64, h, 0.0).astype(jnp.bfloat16)

    class Scatter:
        def __init__(self, n, wd, finish):
            self.n, self.wd, self.finish = n, wd, finish

        def product(self, which, j):
            w = self.wd[2 * j : 2 * j + 2].reshape(CH, DK)
            return lax.dot_general(
                hid[which], w, (((1,), (1,)), ((), ())), preferred_element_type=jnp.float32
            )

        def s0(self, j):
            h = self.n - 1
            sb[h, j] = self.product(oc, j).astype(jnp.bfloat16).reshape(4, ROWS, CH)
            net.send((self.n, "r0", j), sb.at[h, j], rb.at[h, j], sib)
            keep[j] = self.product(c, j).reshape(4, ROWS, CH)

        def chip(self, j, k):
            h = self.n - 1
            return keep[j, xx(k)] + rb[h, j, xx(k)].astype(jnp.float32)

        def s1(self, j):
            h = self.n - 1
            net.recv((self.n, "r0", j), rb.at[h, j], sib)
            u1[h, j] = self.chip(j, 2).astype(jnp.bfloat16)
            for d in (1, -1):
                at = 0 if d == 1 else 64
                net.send(
                    (self.n, "r1", d, j), u1.at[h, j, pl.ds(at, 64)], r1.at[h, j, pl.ds(at, 64)], xdev[d]
                )

        def s2(self, j):
            h = self.n - 1
            for d in (1, -1):
                at, other = (0, 64) if d == 1 else (64, 0)
                part = r1.at[h, j, pl.ds(at, 64)]
                net.recv((self.n, "r1", d, j), part, xdev[-d])
                near = self.chip(j, d)
                both = near[at : at + 64] + part[...].astype(jnp.float32)
                e = 0 if d == 1 else 1
                u2[h, j, e, at : at + 64] = both.astype(jnp.bfloat16)
                u2[h, j, e, other : other + 64] = near[other : other + 64].astype(jnp.bfloat16)
                net.send((self.n, "r2", d, j), u2.at[h, j, e], r2.at[h, j, e], xdev[d])

        def s3(self, j):
            h = self.n - 1
            for d in (1, -1):
                net.recv((self.n, "r2", d, j), r2.at[h, j, 0 if d == 1 else 1], xdev[-d])
            total = self.chip(j, 0) + r2[h, j, 0].astype(jnp.float32) + r2[h, j, 1].astype(jnp.float32)
            self.finish(j, total)

    def cols(j):
        return slice(CH * j, CH * j + CH)

    def to_middle(j, total):
        mid[:, cols(j)] = (xown[:, cols(j)].astype(jnp.float32) + 0.5 * total).astype(jnp.bfloat16)

    def to_result(j, total):
        out_ref[:, cols(j)] = (mid[:, cols(j)].astype(jnp.float32) + 0.5 * total).astype(jnp.bfloat16)

    ga, gb = Gather(1, xn1), Gather(2, xn2)
    ra, rbk = Scatter(1, wd1, to_middle), Scatter(2, wd2, to_result)

    local[0].wait()
    w1.b1_start()
    local[1].wait()
    w1.a1_start()
    w1.h1(0)
    local[2].wait()
    ga.put(xown, gain1)
    for s in range(4):
        ga.g0(s)
    w1.piece(1)
    w1.piece(2)
    w1.a1_forward()
    w1.h2(0)
    ga.g1(0)
    w1.a2_start()
    w1.piece(3)
    w1.piece(4)
    ga.g1(1)
    w1.h2(1)
    w1.h2(2)
    w1.a2_hop(1)
    ga.g1(2)
    ga.g2(0)
    w1.piece(5)
    w1.piece(6)
    ga.g1(3)
    ga.g2(1)
    w1.h2(3)
    w1.h2(4)
    w1.a2_hop(2)
    w1.piece(7)
    ga.g2(2)
    ga.g2(3)
    local[3].wait()
    local[4].wait()
    w2.b1_start()
    w2.a1_start()
    for s in range(4):
        ga.g3(s)
    w1.h2(5)
    w1.h2(6)
    gate_up(xn1, wg1, 0)
    w1.a2_hop(3)
    w1.h2(7)
    gate_up(xn1, wg1, 1)
    w2.a1_forward()
    w2.h1(0)
    w2.piece(1)
    w2.piece(2)
    gate_up(xn1, wg1, 2)
    for i in range(8):
        w1.h2_wait(i)
    gate_up(xn1, wg1, 3)
    w1.a2_hop(4)
    w2.a2_start()
    activate()

    steps = [
        lambda: (w2.piece(3), w2.piece(4)),
        lambda: (w2.h2(0), w2.a2_hop(1)),
        lambda: (w2.piece(5), w2.piece(6)),
        lambda: (w2.h2(1), w2.h2(2)),
        lambda: (w2.piece(7), w2.a2_hop(2)),
        lambda: (w2.h2(3), w2.h2(4)),
        lambda: w2.a2_hop(3),
        lambda: (w2.h2(5), w2.h2(6)),
        lambda: w2.a2_hop(4),
        lambda: w2.h2(7),
    ]
    for t in range(7):
        for stage, do in ((3, ra.s3), (2, ra.s2), (1, ra.s1), (0, ra.s0)):
            if 0 <= t - stage < 4:
                do(t - stage)
        if steps:
            steps.pop(0)()

    gb.put(mid, gain2)
    for s in range(4):
        gb.g0(s)
    for t in range(6):
        if t < 4:
            gb.g1(t)
        if steps:
            steps.pop(0)()
        if 0 <= t - 1 < 4:
            gb.g2(t - 1)
        if 0 <= t - 2 < 4:
            gb.g3(t - 2)
            if t - 2 == 3:
                for i in range(8):
                    w2.h2_wait(i)
            gate_up(xn2, wg2, t - 2)
    activate()
    for t in range(7):
        for stage, do in ((3, rbk.s3), (2, rbk.s2), (1, rbk.s1), (0, rbk.s0)):
            if 0 <= t - stage < 4:
                do(t - stage)
    net.finish()


def layer(x, gu1, d1, gu2, d2, gain1, gain2):
    bf, f32 = jnp.bfloat16, jnp.float32
    hbm = pl.BlockSpec(memory_space=pl.ANY)
    vmem = pl.BlockSpec(memory_space=pltpu.VMEM)
    return pl.pallas_call(
        kernel,
        out_shape=jax.ShapeDtypeStruct((ROWS, D), bf),
        in_specs=[hbm] * 5 + [vmem] * 2,
        out_specs=vmem,
        scratch_shapes=[
            pltpu.VMEM((ROWS, D), bf),
            pltpu.VMEM((ROWS, D), bf),
            pltpu.VMEM((NY, NZ, 64, GU), bf),
            pltpu.VMEM((NY, NZ, 64, GU), bf),
            pltpu.VMEM((NZ, NY, 64, DK), bf),
            pltpu.VMEM((NZ, NY, 64, DK), bf),
            pltpu.VMEM((4, 2, NX, ROWS, CH), bf),
            pltpu.VMEM((4, 2, NX, ROWS, CH), bf),
            pltpu.VMEM((2, 4 * ROWS, GU), f32),
            pltpu.VMEM((2, 4 * ROWS, DK), bf),
            pltpu.VMEM((4, NX, ROWS, CH), f32),
            pltpu.VMEM((2, 4, NX, ROWS, CH), bf),
            pltpu.VMEM((2, 4, NX, ROWS, CH), bf),
            pltpu.VMEM((2, 4, ROWS, CH), bf),
            pltpu.VMEM((2, 4, 2, ROWS, CH), bf),
            pltpu.VMEM((2, 4, ROWS, CH), bf),
            pltpu.VMEM((2, 4, 2, ROWS, CH), bf),
            pltpu.SemaphoreType.DMA((5,)),
            pltpu.SemaphoreType.DMA((SEMS,)),
            pltpu.SemaphoreType.DMA((SEMS,)),
        ],
        compiler_params=pltpu.CompilerParams(
            collective_id=0, has_side_effects=True, vmem_limit_bytes=60 * 2**20
        ),
    )(x, gu1, d1, gu2, d2, gain1, gain2)


def joined(gate, up):
    return jnp.concatenate([gate[:, :512], up[:, :512], gate[:, 512:], up[:, 512:]], axis=1)


def turned(down):
    return jnp.pad(down.T, ((0, 0), (0, DK - H)))


def on_device(tokens, norm_one, gate_one, up_one, down_one, norm_two, gate_two, up_two, down_two):
    return layer(
        tokens,
        joined(gate_one, up_one),
        turned(down_one),
        joined(gate_two, up_two),
        turned(down_two),
        norm_one.reshape(1, D),
        norm_two.reshape(1, D),
    )


def solution(mesh):
    return jax.shard_map(
        on_device,
        mesh=mesh,
        in_specs=(
            P(("fs", "tp"), None),
            P(),
            P("fs", "tp"),
            P("fs", "tp"),
            P("tp", "fs"),
            P(),
            P("fs", "tp"),
            P("fs", "tp"),
            P("tp", "fs"),
        ),
        out_specs=P(("fs", "tp"), None),
        check_vma=False,
    )
```

```python
import math

import jax
import jax.numpy as jnp
from jax import lax
from jax.experimental import pallas as pl
from jax.experimental.pallas import tpu as pltpu
from jax.sharding import PartitionSpec as P

MESH = pl.DeviceIdType.MESH
EPS = 1e-06
NZ, NY, NX = 8, 4, 4
ROWS, D = 128, 2048
GA, GB = 512, 640
DA, DB = 256, 384
DK, H = DA + DB, 576
CH = 512
SEMS = 320

PER_BYTE = 1 / 46.6e3
PER_BYTE_CHIP = 1 / 500e3
HOP, HOP_CHIP = 1.9, 1.1
BACKLOG = 1.5


class Plan:
    def __init__(self):
        self.tasks = {}

    def add(self, name, rank, recv=(), work=None, time=0.0, send=(), after=()):
        self.tasks[name] = (rank, recv, work, time, send, after)

    def order(self):
        now, free, done, arrive, left, result = 0.0, {}, set(), {}, dict(self.tasks), []
        while left:
            pick, later = None, []
            for name, (rank, recv, work, time, send, after) in left.items():
                if not all(a in done for a in after) or not all(r[0] in arrive for r in recv):
                    continue
                at = max([arrive[r[0]] for r in recv], default=0.0)
                at = max([at] + [free.get(s[4], 0.0) - BACKLOG for s in send])
                if at > now:
                    later.append(at)
                elif pick is None or (rank, len(result)) < pick[:2]:
                    pick = (rank, len(result), name)
            if pick is None:
                now = min(later)
                continue
            name = pick[2]
            rank, recv, work, time, send, after = left.pop(name)
            now += time + 0.02
            for key, src, dst, device, link in send:
                size = 2 * math.prod(src.shape)
                start = max(free.get(link, 0.0), now)
                free[link] = start + size * (PER_BYTE_CHIP if link == "c" else PER_BYTE)
                arrive[key] = free[link] + (HOP_CHIP if link == "c" else HOP)
            done.add(name)
            result.append(name)
        self.model_time = now
        return result


class Net:
    def __init__(self, send_sems, recv_sems):
        self.send_sems, self.recv_sems = send_sems, recv_sems
        self.index, self.sent = {}, []

    def copy(self, key, src, dst, device):
        k = self.index.setdefault(key, len(self.index))
        return pltpu.make_async_remote_copy(
            src_ref=src,
            dst_ref=dst,
            send_sem=self.send_sems.at[k],
            recv_sem=self.recv_sems.at[k],
            device_id=device,
            device_id_type=MESH,
        )

    def send(self, key, src, dst, device):
        copy = self.copy(key, src, dst, device)
        copy.start()
        self.sent.append(copy)

    def recv(self, key, ref, device):
        self.copy(key, ref, ref, device).wait_recv()

    def finish(self):
        for copy in self.sent:
            copy.wait_send()


def kernel(
    x_in, gate1_in, up1_in, down1_in, gate2_in, up2_in, down2_in, rest_in, gain1, gain2, out_ref,
    xown, mid, ga1, gb1, ga2, gb2, da1, db1, da2, db2, xn1, xn2, acca, accb, hid, keep,
    sb, rb, u1, u2, r1, r2, local_sems, send_sems, recv_sems,
):
    fs, tp = lax.axis_index("fs"), lax.axis_index("tp")
    z, y = lax.div(fs, NY), lax.rem(fs, NY)
    x, c = lax.div(tp, 2), lax.rem(tp, 2)
    oc = 1 - c

    zs = {k: lax.rem(z + k + NZ, NZ) for k in range(-4, 5)}
    ys = {k: lax.rem(y + k + NY, NY) for k in range(-1, 3)}
    xs = {k: lax.rem(x + k + NX, NX) for k in range(-1, 3)}
    zdev = {s: (zs[s] * NY + y, tp) for s in (1, -1)}
    ydev = {s: (z * NY + ys[s], tp) for s in (1, -1)}
    xdev = {s: (fs, xs[s] * 2 + c) for s in (1, -1)}
    sib = (fs, x * 2 + oc)
    net, plan = Net(send_sems, recv_sems), Plan()

    def fetch(k, src, dst):
        copy = pltpu.make_async_copy(src, dst, local_sems.at[k])
        copy.start()
        return copy

    def lanes(ref, at, size):
        return ref.at[:, pl.ds(at, size)]

    local = {
        1: [
            fetch(0, lanes(gate1_in, 0, 512), ga1.at[y, z]),
            fetch(1, lanes(up1_in, 0, 512), lanes(gb1.at[y, z], 0, 512)),
            fetch(2, lanes(rest_in, 0, 128), lanes(gb1.at[y, z], 512, 128)),
        ],
        0: [fetch(3, x_in, xown)],
        2: [fetch(4, lanes(down1_in, 0, DA), da1.at[z, y]), fetch(5, lanes(rest_in, 128, DB), db1.at[z, y])],
        3: [
            fetch(6, lanes(gate2_in, 0, 512), ga2.at[y, z]),
            fetch(7, lanes(up2_in, 0, 512), lanes(gb2.at[y, z], 0, 512)),
            fetch(8, lanes(rest_in, 512, 128), lanes(gb2.at[y, z], 512, 128)),
        ],
        4: [fetch(9, lanes(down2_in, 0, DA), da2.at[z, y]), fetch(10, lanes(rest_in, 640, DB), db2.at[z, y])],
    }

    barrier = pltpu.get_barrier_semaphore()
    for dev in (*zdev.values(), *ydev.values(), *xdev.values(), sib):
        pl.semaphore_signal(barrier, inc=1, device_id=dev, device_id_type=MESH)
    pl.semaphore_wait(barrier, 7)

    def origin(i):
        return (1, (i + 1) // 2) if i % 2 else (-1, i // 2)

    def weights(m, part_a, pair_a, part_b):
        def land():
            for copy in local[m]:
                copy.wait()

        own_a, own_b = part_a(y, z), part_b(y, z)
        plan.add((m, "land"), m, work=land)
        plan.add(
            (m, "b1s"), m, after=[(m, "land")],
            send=[((m, "b1", s, 1), own_b, own_b, zdev[s], f"z{s}") for s in (1, -1)],
        )
        plan.add(
            (m, "a1s"), m, after=[(m, "land")],
            send=[((m, "a1", s), own_a, own_a, ydev[s], f"y{s}") for s in (1, -1)],
        )
        plan.add(
            (m, "h1", 0), m + 0.1, after=[(m, "land")],
            send=[((m, "h1", s, 0), own_b, own_b, ydev[s], f"y{s}") for s in (1, -1)],
        )
        for i in range(1, 8):
            s, k = origin(i)
            ref = part_b(y, zs[-s * k])
            more = k < (4 if s == 1 else 3)
            plan.add(
                (m, "b1", i), m, recv=[((m, "b1", s, k), ref, zdev[-s])],
                send=[((m, "b1", s, k + 1), ref, ref, zdev[s], f"z{s}")] if more else [],
            )
            plan.add(
                (m, "h1", i), m + 0.1, after=[(m, "b1", i)],
                send=[((m, "h1", e, i), ref, ref, ydev[e], f"y{e}") for e in (1, -1)],
            )
        for i in range(8):
            s, k = origin(i)
            o = zs[-s * k]
            for e in (1, -1):
                ref = part_b(ys[-e], o)
                forward = (i % 2 == 0) == (e == 1)
                plan.add(
                    (m, "h2", e, i), m, recv=[((m, "h1", e, i), ref, ydev[-e])],
                    send=[((m, "h2", i), ref, ref, ydev[e], f"y{e}")] if forward else [],
                )
            plan.add(
                (m, "h2w", i), m + 0.3,
                recv=[((m, "h2", i), part_b(ys[2], o), ydev[-1 if i % 2 == 0 else 1])],
            )
        ref = part_a(ys[-1], z)
        plan.add(
            (m, "a1", 1), m, recv=[((m, "a1", 1), ref, ydev[-1])],
            send=[((m, "a1f"), ref, ref, ydev[1], "y1")],
        )
        plan.add((m, "a1", -1), m, recv=[((m, "a1", -1), part_a(ys[1], z), ydev[1])])
        plan.add((m, "a1", 2), m, recv=[((m, "a1f"), part_a(ys[2], z), ydev[-1])])
        for q in (0, 1):
            for s, last in ((-1, 4), (1, 3)):
                ref = pair_a(q, z)
                plan.add(
                    (m, "a2", s, q, 0), m + 0.05, after=[(m, "land")] + [(m, "a1", k) for k in (1, -1, 2)],
                    send=[((m, "a2", s, q, 1), ref, ref, zdev[s], f"z{s}")],
                )
                for k in range(1, last + 1):
                    ref = pair_a(q, zs[-s * k])
                    plan.add(
                        (m, "a2", s, q, k), m + 0.05, recv=[((m, "a2", s, q, k), ref, zdev[-s])],
                        send=[((m, "a2", s, q, k + 1), ref, ref, zdev[s], f"z{s}")] if k < last else [],
                    )

    def gate_parts(a, b):
        return (
            lambda yi, zi: a.at[yi, zi],
            lambda q, zi: a.at[pl.ds(2 * q, 2), zi],
            lambda yi, zi: b.at[yi, zi],
        )

    def down_parts(a, b):
        return (
            lambda yi, zi: a.at[zi, yi],
            lambda q, zi: a.at[zi, pl.ds(2 * q, 2)],
            lambda yi, zi: b.at[zi, yi],
        )

    weights(1, *gate_parts(ga1, gb1))
    weights(2, *down_parts(da1, db1))
    weights(3, *gate_parts(ga2, gb2))
    weights(4, *down_parts(da2, db2))

    offsets = (0, -1, 1, 2)

    def gather(n, src, gain, xn, after):
        def norm():
            if n == 1:
                local[0][0].wait()
            lane = lax.broadcasted_iota(jnp.int32, (32, 128), 1)

            @pl.loop(0, ROWS // 32)
            def _(b):
                rows = pl.ds(pl.multiple_of(b * 32, 32), 32)
                v = src[rows, :].astype(jnp.float32)
                mean = jnp.mean(v * v, axis=-1, keepdims=True)
                scaled = v * lax.rsqrt(mean + EPS) * gain[...]
                for j in range(4):
                    for i in range(4):
                        at = 512 * i + 128 * (j // 2)
                        one, two = scaled[:, at : at + 128], scaled[:, at + 256 : at + 384]
                        if j % 2 == 0:
                            tile = jnp.where(lane < 64, one, pltpu.roll(two, 64, 1))
                        else:
                            tile = jnp.where(lane < 64, pltpu.roll(one, 64, 1), two)
                        xn[j, c, x, rows, 128 * i : 128 * i + 128] = tile.astype(jnp.bfloat16)

        plan.add((n, "norm"), 0.5, work=norm, time=0.9, after=after)
        for s in range(4):
            j = ys[offsets[s]]
            own = xn.at[j, c, x]
            plan.add(
                (n, "g0", s), 0.1 * s, after=[(n, "norm")],
                send=[((n, "g1", d, s), own, own, xdev[d], f"x{d}") for d in (1, -1)]
                + [((n, "gs", 0, s), own, own, sib, "c")],
            )
            halves = []
            for d in (1, -1):
                ref = xn.at[j, c, xs[-d]]
                half = xn.at[j, c, xs[-d], pl.ds(0 if d == 1 else 64, 64)]
                plan.add(
                    (n, "g1", d, s), 0.1 * s, recv=[((n, "g1", d, s), ref, xdev[-d])],
                    send=[((n, "g2", d, s), half, half, xdev[d], f"x{d}"), ((n, "gs", d, s), ref, ref, sib, "c")],
                )
                halves.append(
                    ((n, "g2", d, s), xn.at[j, c, xs[2], pl.ds(0 if d == 1 else 64, 64)], xdev[-d])
                )
            ref = xn.at[j, c, xs[2]]
            plan.add((n, "g2", s), 0.1 * s, recv=halves, send=[((n, "gs", 2, s), ref, ref, sib, "c")])
            plan.add(
                (n, "g3", s), 0.5,
                recv=[
                    ((n, "gs", d, s), xn.at[j, oc, xs[k]], sib)
                    for d, k in ((0, 0), (1, -1), (-1, 1), (2, 2))
                ],
            )

    def hidden(n, m, xn, ga, gb, after):
        started = set()

        def dot(acc, w, s):
            j = ys[offsets[s]]
            first = acc not in started
            started.add(acc)
            target = acca if acc == "a" else accb

            @pl.loop(0, 2)
            def _(i):
                rows = xn[j, i].reshape(4 * ROWS, CH)
                part = jnp.dot(rows, w[j].reshape(CH, w.shape[-1]), preferred_element_type=jnp.float32)
                if first:
                    target[i] = part
                else:
                    target[i] += part

        parts = {
            0: [(m, "land")] + [(m, "b1", i) for i in range(1, 8)],
            1: [(m, "h2", 1, i) for i in range(8)],
            2: [(m, "h2", -1, i) for i in range(8)],
            3: [(m, "h2w", i) for i in range(8)],
        }
        blocks = [(m, "a2", s, q, k) for q in (0, 1) for s, last in ((-1, 4), (1, 3)) for k in range(last + 1)]
        for s in range(4):
            plan.add(
                (n, "gub", s), 5, work=lambda s=s: dot("b", gb, s), time=0.98,
                after=[(n, "norm"), (n, "g2", s), (n, "g3", s)] + parts[s] + after,
            )
            plan.add(
                (n, "gua", s), 5, work=lambda s=s: dot("a", ga, s), time=0.8,
                after=[(n, "norm"), (n, "g2", s), (n, "g3", s)] + blocks + after,
            )

        def activate():
            lane = lax.broadcasted_iota(jnp.int32, (64, 128), 1)

            @pl.loop(0, 16)
            def _(b):
                i, rows = lax.div(b, 8), pl.ds(pl.multiple_of(lax.rem(b, 8) * 64, 64), 64)
                for k in range(4):
                    g = acca[i, rows, 128 * k : 128 * k + 128]
                    u = accb[i, rows, 128 * k : 128 * k + 128]
                    h = g / (1.0 + jnp.exp(-g)) * u
                    hid[i, rows, 128 * k : 128 * k + 128] = h.astype(jnp.bfloat16)
                t = accb[i, rows, 512:640]
                h = t / (1.0 + jnp.exp(-t)) * pltpu.roll(t, 64, 1)
                hid[i, rows, 512:640] = jnp.where(lane < 64, h, 0.0).astype(jnp.bfloat16)

        plan.add(
            (n, "act"), 5, work=activate, time=1.25,
            after=[(n, k, s) for k in ("gua", "gub") for s in range(4)],
        )

    def scatter(n, m, da, db, add):
        h = n - 1

        def product(which, i):
            s, k = origin(i)
            o = zs[-s * k]
            dims = (((1,), (1,)), ((), ()))
            return lax.dot_general(
                hid[which, :, 0:DA], da[o].reshape(256, DA), dims, preferred_element_type=jnp.float32
            ) + lax.dot_general(
                hid[which, :, DA:DK], db[o].reshape(256, DB), dims, preferred_element_type=jnp.float32
            )

        def give(j):
            for b in (0, 1):
                sb[h, j, b] = product(oc, 2 * j + b).astype(jnp.bfloat16).reshape(4, ROWS, 256)

        def hold(j):
            for b in (0, 1):
                keep[j, b] = product(c, 2 * j + b).reshape(4, ROWS, 256)

        def chip(j, b, k, rows):
            return keep[j, b, xs[k], rows] + rb[h, j, b, xs[k], rows].astype(jnp.float32)

        every, low, high = slice(0, 128), slice(0, 64), slice(64, 128)

        def far(j):
            for b in (0, 1):
                u1[h, j, 0, b] = chip(j, b, 2, low).astype(jnp.bfloat16)
                u1[h, j, 1, b] = chip(j, b, 2, high).astype(jnp.bfloat16)

        def near(j, d):
            e, some, rest = (0, low, high) if d == 1 else (1, high, low)
            for b in (0, 1):
                both = chip(j, b, d, some) + r1[h, j, e, b].astype(jnp.float32)
                u2[h, j, e, b, some] = both.astype(jnp.bfloat16)
                u2[h, j, e, b, rest] = chip(j, b, d, rest).astype(jnp.bfloat16)

        def last(j):
            for b in (0, 1):
                s, k = origin(2 * j + b)
                cols = pl.ds(pl.multiple_of(zs[-s * k] * 256, 256), 256)
                total = chip(j, b, 0, every)
                total += r2[h, j, 0, b].astype(jnp.float32) + r2[h, j, 1, b].astype(jnp.float32)
                add(cols, total)

        for j in range(4):
            needs = [(n, "act")]
            for i in (2 * j, 2 * j + 1):
                s, k = origin(i)
                s = -1 if k == 4 else s
                needs += [(m, "a2", s, q, k) for q in (0, 1)]
                needs += [(m, "b1", i) if i else (m, "land")]
                needs += [(m, "h2", 1, i), (m, "h2", -1, i), (m, "h2w", i)]
            plan.add(
                (n, "s0", j), 0.5 + 0.1 * j, work=lambda j=j: give(j), time=0.62, after=needs,
                send=[((n, "r0", j), sb.at[h, j], rb.at[h, j], sib, "c")],
            )
            plan.add((n, "s0k", j), 0.5 + 0.1 * j, work=lambda j=j: hold(j), time=0.62, after=[(n, "s0", j)])
            plan.add(
                (n, "s1", j), 0.2, recv=[((n, "r0", j), rb.at[h, j], sib)], after=[(n, "s0k", j)],
                work=lambda j=j: far(j), time=0.05,
                send=[
                    ((n, "r1", d, j), u1.at[h, j, 0 if d == 1 else 1], r1.at[h, j, 0 if d == 1 else 1], xdev[d], f"x{d}")
                    for d in (1, -1)
                ],
            )
            for d in (1, -1):
                e = 0 if d == 1 else 1
                plan.add(
                    (n, "s2", d, j), 0.1, recv=[((n, "r1", d, j), r1.at[h, j, e], xdev[-d])],
                    after=[(n, "s1", j)], work=lambda j=j, d=d: near(j, d), time=0.05,
                    send=[((n, "r2", d, j), u2.at[h, j, e], r2.at[h, j, e], xdev[d], f"x{d}")],
                )
            plan.add(
                (n, "s3", j), 0.3,
                recv=[((n, "r2", d, j), r2.at[h, j, 0 if d == 1 else 1], xdev[-d]) for d in (1, -1)],
                after=[(n, "s1", j)], work=lambda j=j: last(j), time=0.1,
            )

    def to_middle(cols, total):
        mid[:, cols] = (xown[:, cols].astype(jnp.float32) + 0.5 * total).astype(jnp.bfloat16)

    def to_result(cols, total):
        out_ref[:, cols] = (mid[:, cols].astype(jnp.float32) + 0.5 * total).astype(jnp.bfloat16)

    gather(1, xown, gain1, xn1, [(1, "b1s"), (1, "a1s"), (1, "h1", 0)])
    hidden(1, 1, xn1, ga1, gb1, [])
    scatter(1, 2, da1, db1, to_middle)
    gather(2, mid, gain2, xn2, [(1, "s3", j) for j in range(4)])
    hidden(2, 3, xn2, ga2, gb2, [(1, "act")])
    scatter(2, 4, da2, db2, to_result)

    for name in plan.order():
        rank, recv, work, time, send, after = plan.tasks[name]
        with jax.named_scope("_".join(str(p) for p in name)):
            for key, ref, device in recv:
                net.recv(key, ref, device)
            if work is not None:
                work()
            for key, src, dst, device, link in send:
                net.send(key, src, dst, device)
    net.finish()


def layer(*args):
    bf, f32 = jnp.bfloat16, jnp.float32
    hbm = pl.BlockSpec(memory_space=pl.ANY)
    vmem = pl.BlockSpec(memory_space=pltpu.VMEM)
    pair = (2, 4, 2)
    return pl.pallas_call(
        kernel,
        out_shape=jax.ShapeDtypeStruct((ROWS, D), bf),
        in_specs=[hbm] * 8 + [vmem] * 2,
        out_specs=vmem,
        scratch_shapes=[
            pltpu.VMEM((ROWS, D), bf),
            pltpu.VMEM((ROWS, D), bf),
            pltpu.VMEM((NY, NZ, 64, GA), bf),
            pltpu.VMEM((NY, NZ, 64, GB), bf),
            pltpu.VMEM((NY, NZ, 64, GA), bf),
            pltpu.VMEM((NY, NZ, 64, GB), bf),
            pltpu.VMEM((NZ, NY, 64, DA), bf),
            pltpu.VMEM((NZ, NY, 64, DB), bf),
            pltpu.VMEM((NZ, NY, 64, DA), bf),
            pltpu.VMEM((NZ, NY, 64, DB), bf),
            pltpu.VMEM((4, 2, NX, ROWS, CH), bf),
            pltpu.VMEM((4, 2, NX, ROWS, CH), bf),
            pltpu.VMEM((2, 4 * ROWS, GA), f32),
            pltpu.VMEM((2, 4 * ROWS, GB), f32),
            pltpu.VMEM((2, 4 * ROWS, DK), bf),
            pltpu.VMEM((4, 2, NX, ROWS, 256), f32),
            pltpu.VMEM((*pair, NX, ROWS, 256), bf),
            pltpu.VMEM((*pair, NX, ROWS, 256), bf),
            pltpu.VMEM((*pair, 2, ROWS // 2, 256), bf),
            pltpu.VMEM((*pair, 2, ROWS, 256), bf),
            pltpu.VMEM((*pair, 2, ROWS // 2, 256), bf),
            pltpu.VMEM((*pair, 2, ROWS, 256), bf),
            pltpu.SemaphoreType.DMA((11,)),
            pltpu.SemaphoreType.DMA((SEMS,)),
            pltpu.SemaphoreType.DMA((SEMS,)),
        ],
        compiler_params=pltpu.CompilerParams(
            collective_id=0, has_side_effects=True, vmem_limit_bytes=60 * 2**20
        ),
    )(*args)


def on_device(tokens, norm_one, gate_one, up_one, down_one, norm_two, gate_two, up_two, down_two):
    def rest(gate, up, turned):
        return [gate[:, 512:], up[:, 512:], turned[:, DA:], jnp.zeros((64, DK - H), turned.dtype)]

    turned_one, turned_two = down_one.T, down_two.T
    parts = jnp.concatenate(rest(gate_one, up_one, turned_one) + rest(gate_two, up_two, turned_two), axis=1)
    return layer(
        tokens, gate_one, up_one, turned_one, gate_two, up_two, turned_two, parts,
        norm_one.reshape(1, D), norm_two.reshape(1, D),
    )


def solution(mesh):
    return jax.shard_map(
        on_device,
        mesh=mesh,
        in_specs=(
            P(("fs", "tp"), None),
            P(),
            P("fs", "tp"),
            P("fs", "tp"),
            P("tp", "fs"),
            P(),
            P("fs", "tp"),
            P("fs", "tp"),
            P("tp", "fs"),
        ),
        out_specs=P(("fs", "tp"), None),
        check_vma=False,
    )
```

```python
import math

import jax
import jax.numpy as jnp
from jax import lax
from jax.experimental import pallas as pl
from jax.experimental.pallas import tpu as pltpu
from jax.sharding import PartitionSpec as P

MESH = pl.DeviceIdType.MESH
EPS = 1e-06
NZ, NY, NX = 8, 4, 4
ROWS, D = 128, 2048
GA, GB = (512, 384), (640, 768)
DK, H = 640, 576
DROWS = 80
CH = 512
RING = 6
LINKS = ("z1", "z-1", "y1", "y-1", "x1", "x-1", "c")
SEMS = 268
J, NB = 4, 2

PER_BYTE = 1 / 46600.0
PER_BYTE_CHIP = 1 / 500e3
HOP, HOP_CHIP = 2.3, 1.1
RANK = {
    "s0": 4.94,
    "act": 2,
    "s1": -9.475,
    "s2": -1.164,
    "s3": -8.896,
    "g": -9.746,
    "b1": -7.67,
    "a1s": 0.115,
    "a1": -2.264,
    "h1": -1.386,
    "h2": 7.127,
    "h2w": 3.196,
    "a2": 1.94,
    "a2k": 0.2,
    "bi": 0.1,
    "bx": 1,
    "gub": 5,
    "gua": 5,
}
RANK_OF_MATRIX = {1: 1, 2: -6.866, 3: 3.774, 4: -3.291}
SLACK = {1: 2.5, 2: 1.5, 3: 1.5, 4: 0.6}
ACTIVATION_KINDS = (
    "spread", "norm", "g0", "g1", "g2", "g3", "gub", "gua", "act", "s0", "s0k", "s1", "s2", "s3"
)


def rank_of(name):
    kind = name[1]
    if kind in ("gub", "gua", "act"):
        return RANK[kind] + 0.1 * name[2]
    if kind in ("s0", "s0k"):
        return RANK["s0"] + 0.1 * name[2] + 0.02 * name[3]
    if kind in ("s1", "s2", "s3"):
        return RANK[kind]
    if kind in ("norm", "g0", "g1", "g2", "g3"):
        return RANK["g"]
    if kind == "spread":
        return 1.0 + name[2]
    rank = RANK_OF_MATRIX[name[0]] + RANK[{"land": "b1", "b1s": "b1", "h1w": "h2", "a2w": "a2"}.get(kind, kind)]
    if kind == "a2":
        return rank + RANK["a2k"] * name[4]
    return rank + (RANK["bi"] * name[-1] if kind in ("b1", "h1", "h2") else 0.0)


class Plan:
    def __init__(self, net):
        self.tasks, self.net = {}, net

    def add(self, name, recv=(), work=None, time=0.0, send=(), after=()):
        self.tasks[name] = (recv, work, time, send, after)
        for keys, ref, device in recv:
            self.net.expect(keys)

    def order(self):
        now, free, done, arrive, left = 0.0, {}, {}, {}, dict(self.tasks)
        while left:
            pick, later = None, []
            for name, (recv, work, time, send, after) in left.items():
                if not all(a in done for a in after) or not all(key in arrive for r in recv for key in r[0]):
                    continue
                slack = RANK["bx"] if name[1] in ACTIVATION_KINDS else SLACK[name[0]]
                at = max([arrive[key] for r in recv for key in r[0]] + [free.get(s[4], 0.0) - slack for s in send], default=0.0)
                if at > now + 1e-9:
                    later.append(at)
                elif pick is None or rank_of(name) < pick[0]:
                    pick = (rank_of(name), name)
            if pick is None:
                now = min(later)
                continue
            name = pick[1]
            recv, work, time, send, after = left.pop(name)
            now += time + 0.02
            for key, src, dst, device, link in send:
                size = 2 * math.prod(src.shape)
                start = max(free.get(link, 0.0), now)
                free[link] = start + size * (PER_BYTE_CHIP if link == "c" else PER_BYTE)
                arrive[key] = free[link] + (HOP_CHIP if link == "c" else HOP)
            done[name] = now
        self.model = done
        return list(done)


class Net:
    def __init__(self, send_sems, recv_sems):
        self.send_sems, self.recv_sems = send_sems, recv_sems
        self.index, self.sent = {}, {link: [] for link in LINKS}

    def expect(self, keys):
        k = len(set(self.index.values()))
        self.index.update({key: k for key in keys})

    def copy(self, key, src, dst, device, ring):
        return pltpu.make_async_remote_copy(
            src_ref=src,
            dst_ref=dst,
            send_sem=self.send_sems.at[ring],
            recv_sem=self.recv_sems.at[self.index[key]],
            device_id=device,
            device_id_type=MESH,
        )

    def send(self, key, src, dst, device, link):
        sent = self.sent[link]
        if len(sent) >= RING:
            sent[-RING].wait_send()
        copy = self.copy(key, src, dst, device, RING * LINKS.index(link) + len(sent) % RING)
        copy.start()
        sent.append(copy)

    def recv(self, keys, ref, device):
        self.copy(keys[0], ref, ref, device, 0).wait_recv()

    def finish(self):
        for sent in self.sent.values():
            for copy in sent[-RING:]:
                copy.wait_send()


def kernel(
    x_in, gate1_in, up1_in, down1_in, gate2_in, up2_in, down2_in, gain1_in, gain2_in, out_hbm,
    gain1, gain2, tails, turned, xown, mid, out, ga1, gb1, ga2, gb2, da1, db1, da2, db2, xn1, xn2, acca, accb, hid, ends,
    keep, sb, rb, u1, u2, r1, r2, local_sems, send_sems, recv_sems,
):
    fs, tp = lax.axis_index("fs"), lax.axis_index("tp")
    z, y = lax.div(fs, NY), lax.rem(fs, NY)
    x, c = lax.div(tp, 2), lax.rem(tp, 2)
    oc = 1 - c

    zs = {k: lax.rem(z + k + NZ, NZ) for k in range(-4, 5)}
    ys = {k: lax.rem(y + k + NY, NY) for k in range(-1, 3)}
    xs = {k: lax.rem(x + k + NX, NX) for k in range(-1, 3)}
    zdev = {s: (zs[s] * NY + y, tp) for s in (1, -1)}
    ydev = {s: (z * NY + ys[s], tp) for s in (1, -1)}
    xdev = {s: (fs, xs[s] * 2 + c) for s in (1, -1)}
    sib = (fs, x * 2 + oc)
    net = Net(send_sems, recv_sems)
    plan = Plan(net)

    fetches = {}

    def fetch(name, src, dst):
        fetches[name] = pltpu.make_async_copy(src, dst, local_sems.at[len(fetches)])
        fetches[name].start()

    def lanes(ref, at, size):
        return ref.at[:, pl.ds(at, size)]

    def fetch_gate(m, gate_in, up_in, ga, gb):
        h = (m - 1) // 2
        fetch((m, 2), gate_in, tails.at[h, 0])
        fetch((m, 3), up_in, tails.at[h, 1])
        fetch((m, 0), lanes(gate_in, 0, GA[h]), ga.at[y, z])
        fetch((m, 1), lanes(up_in, 0, 512), lanes(gb.at[y, z], 512 - GA[h], 512))

    def fetch_down(m, down_in, da):
        fetch((m, 1), down_in, turned.at[m // 2 - 1])
        fetch((m, 0), lanes(down_in, 0, 256), da.at[z, y])

    def join_gate(m, gb):
        h = (m - 1) // 2
        fetches[m, 2].wait()
        fetches[m, 3].wait()
        if GA[h] < 512:
            gb[y, z, :, 0 : 512 - GA[h]] = tails[h, 0, :, GA[h] : 512]
        gb[y, z, :, GB[h] - 128 : GB[h]] = jnp.concatenate([tails[h, 0, :, 512:576], tails[h, 1, :, 512:576]], axis=1)

    def join_down(m, db):
        fetches[m, 1].wait()
        h = m // 2 - 1
        db[z, y, 0:64] = turned[h, :, 256:512]
        end = turned[h, :, 512:576]
        db[z, y, 64:DROWS] = jnp.concatenate([end[16 * g : 16 * g + 16] for g in range(4)], axis=1)

    fetch_gate(1, gate1_in, up1_in, ga1, gb1)
    fetch_down(2, down1_in, da1)
    fetch("x", x_in, xown)
    fetch("gain1", gain1_in, gain1)
    fetch_gate(3, gate2_in, up2_in, ga2, gb2)
    fetch_down(4, down2_in, da2)
    fetch("gain2", gain2_in, gain2)

    barrier = pltpu.get_barrier_semaphore()
    for dev in (*zdev.values(), *ydev.values(), *xdev.values(), sib):
        pl.semaphore_signal(barrier, inc=1, device_id=dev, device_id_type=MESH)
    join_gate(1, gb1)
    join_down(2, db1)
    join_gate(3, gb2)
    join_down(4, db2)
    pl.semaphore_wait(barrier, 7)

    def origin(i):
        return (1, (i + 1) // 2) if i % 2 else (-1, i // 2)

    def way(m, i):
        return (-1, 4) if i == 7 and m % 2 == 0 else origin(i)

    arrivals = {}

    def weights(m, part_a, part_b, eight_a, eight_b, four_b=None):
        def land():
            fetches[m, 0].wait()
            if m % 2:
                fetches[m, 1].wait()

        own_a, own_b = part_a(y, z), part_b(y, z)
        landed = [(m, "land")]
        plan.add((m, "land"), work=land)
        plan.add(
            (m, "b1s"), after=landed, send=[((m, "b1", s, 1), own_b, own_b, zdev[s], f"z{s}") for s in (1, -1)]
        )
        plan.add((m, "a1s"), after=landed, send=[((m, "a1", s), own_a, own_a, ydev[s], f"y{s}") for s in (1, -1)])
        plan.add(
            (m, "h1", 0), after=landed, send=[((m, "h1", s, 0), own_b, own_b, ydev[s], f"y{s}") for s in (1, -1)]
        )
        far = 1 if m % 2 else -1
        for i in range(1, 8):
            s, k = way(m, i)
            ref = part_b(y, zs[-s * k])
            more = k < (4 if s == far else 3)
            plan.add(
                (m, "b1", i), recv=[([(m, "b1", s, k)], ref, zdev[-s])],
                send=[((m, "b1", s, k + 1), ref, ref, zdev[s], f"z{s}")] if more else [],
            )
            plan.add(
                (m, "h1", i), after=[(m, "b1", i)],
                send=[((m, "h1", e, i), ref, ref, ydev[e], f"y{e}") for e in (1, -1)],
            )
        for i in range(8):
            s, k = origin(i)
            e = 1 if i % 2 == 0 else -1
            ref = part_b(ys[-e], zs[-s * k])
            plan.add(
                (m, "h2", i), recv=[([(m, "h1", e, i)], ref, ydev[-e])],
                send=[((m, "h2", i), ref, ref, ydev[e], f"y{e}")],
            )
        if m % 2:
            for e in (1, -1):
                keys = [(m, "h1", e, i) for i in range(8) if (i % 2 == 0) != (e == 1)]
                plan.add((m, "h1w", e), recv=[(keys, four_b, ydev[-e])])
            plan.add((m, "h2w", 0), recv=[([(m, "h2", i) for i in range(8)], eight_b, ydev[1])])
        else:
            for j in range(J):
                some = range(NB * j, NB * j + NB)
                keys = [(m, "h1", -1 if i % 2 == 0 else 1, i) for i in some] + [(m, "h2", i) for i in some]
                plan.add((m, "h2w", j), recv=[(keys, eight_b, ydev[1])])
        for s in (1, -1):
            ref = part_a(ys[-s], z)
            plan.add(
                (m, "a1", s), recv=[([(m, "a1", s)], ref, ydev[-s])],
                send=[((m, "a1f"), ref, ref, ydev[s], f"y{s}")] if s == far else [],
            )
        plan.add((m, "a1", 2), recv=[([(m, "a1f")], part_a(ys[2], z), ydev[-far])])
        lasts = []
        for u, (row, ready) in enumerate([(0, (m, "land")), (-1, (m, "a1", 1)), (1, (m, "a1", -1)), (2, (m, "a1", 2))]):
            arrivals[m, u, 0] = ready
            for s, last in ((-1, 4 - u % 2), (1, 3 + u % 2)):
                ref = part_a(ys[row], z)
                plan.add(
                    (m, "a2", s, u, 0), after=[ready], send=[((m, "a2", s, u, 1), ref, ref, zdev[s], f"z{s}")]
                )
                for k in range(1, last):
                    ref = part_a(ys[row], zs[-s * k])
                    plan.add(
                        (m, "a2", s, u, k), recv=[([(m, "a2", s, u, k)], ref, zdev[-s])],
                        send=[((m, "a2", s, u, k + 1), ref, ref, zdev[s], f"z{s}")],
                    )
                    arrivals[m, u, -s * k] = (m, "a2", s, u, k)
                lasts.append((m, "a2", s, u, last))
                arrivals[m, u, -4 if last == 4 else -s * last] = (m, "a2w", 0)
        plan.add((m, "a2w", 0), recv=[(lasts, eight_a, zdev[1])])

    def block_needs(m, i):
        s, k = origin(i)
        needs = [(m, "b1", i) if i else (m, "land"), (m, "h2", i), (m, "h2w", i // NB)]
        return needs + [arrivals[m, u, -s * k] for u in range(4)]

    def gate_weights(m, a, b):
        weights(m, lambda yi, zi: a.at[yi, zi], lambda yi, zi: b.at[yi, zi], a.at[0], b.at[0], b.at[0, 0:4])

    def down_weights(m, a, b):
        weights(m, lambda yi, zi: a.at[zi, yi], lambda yi, zi: b.at[zi, yi], a.at[0:2], b.at[0 : NB // 2])

    gate_weights(1, ga1, gb1)
    down_weights(2, da1, db1)
    gate_weights(3, ga2, gb2)
    down_weights(4, da2, db2)

    offsets = (0, -1, 1, 2)

    def gather(n, src, gain, xn):
        waited = []

        def norm(t):
            if not waited:
                waited.append(t)
                if n == 1:
                    fetches["x"].wait()
                fetches[f"gain{n}"].wait()
            lane = lax.broadcasted_iota(jnp.int32, (32, 128), 1)

            @pl.loop(0, 2)
            def _(b):
                rows = pl.ds(pl.multiple_of(64 * t + b * 32, 32), 32)
                v = src[rows, :].astype(jnp.float32)
                mean = jnp.mean(v * v, axis=-1, keepdims=True)
                scaled = v * lax.rsqrt(mean + EPS) * gain[...]
                rows = pl.ds(pl.multiple_of(b * 32, 32), 32)
                for j in range(4):
                    for i in range(4):
                        at = 512 * i + 128 * (j // 2)
                        one, two = scaled[:, at : at + 128], scaled[:, at + 256 : at + 384]
                        if j % 2 == 0:
                            tile = jnp.where(lane < 64, one, pltpu.roll(two, 64, 1))
                        else:
                            tile = jnp.where(lane < 64, pltpu.roll(one, 64, 1), two)
                        xn[t, c, x, rows, 512 * j + 128 * i : 512 * j + 128 * i + 128] = tile.astype(jnp.bfloat16)

        for t in (0, 1):
            if n == 1:
                after = [(1, "land"), (1, "b1s"), (1, "a1s"), (1, "h1", 0)]
            else:
                after = [(1, "s3", t, j) for j in range(J)]
            plan.add((n, "norm", t), work=lambda t=t: norm(t), time=0.5, after=after)
            for p in (0, 1):
                q, part = (t, p), pl.ds(1024 * p, 1024)
                own = xn.at[t, c, x, :, part]
                plan.add(
                    (n, "g0", *q), after=[(n, "norm", t)],
                    send=[((n, "g1", d, *q), own, own, xdev[d], f"x{d}") for d in (1, -1)]
                    + [((n, "gs", 0, *q), own, own, sib, "c")],
                )
                for d in (1, -1):
                    some = pl.ds(0 if d == 1 else 32, 32)
                    ref, half = xn.at[t, c, xs[-d], :, part], xn.at[t, c, xs[-d], some, part]
                    plan.add(
                        (n, "g1", d, *q), recv=[([(n, "g1", d, *q)], ref, xdev[-d])],
                        send=[
                            ((n, "g2", d, *q), half, half, xdev[d], f"x{d}"),
                            ((n, "gs", d, *q), ref, ref, sib, "c"),
                        ],
                    )
                ref = xn.at[t, c, xs[2], :, part]
                plan.add(
                    (n, "g2", *q), recv=[([(n, "g2", d, *q) for d in (1, -1)], ref, xdev[1])],
                    send=[((n, "gs", 2, *q), ref, ref, sib, "c")],
                )
                keys = [(n, "gs", d, *q) for d in (0, 1, -1, 2)]
                plan.add((n, "g3", *q), recv=[(keys, xn.at[t, oc, :, :, part], sib)])

    def hidden(n, m, xn, ga, gb):
        started = set()

        h = n - 1

        def dot(target, w, t, s):
            size = w.shape[-1]
            if n == 2:
                rows = xn[t, :, :, :, 1024 * s : 1024 * s + 1024].reshape(4 * ROWS, 1024)
                part = w[2 * s : 2 * s + 2].reshape(1024, size)
            else:
                j = ys[offsets[s]]
                rows = xn[t, :, :, :, pl.ds(pl.multiple_of(CH * j, CH), CH)].reshape(4 * ROWS, CH)
                part = w[j].reshape(CH, size)
            product = jnp.dot(rows, part, preferred_element_type=jnp.float32)
            if (w is ga, t) in started:
                target[t, :, 0:size] += product
            else:
                target[t, :, 0:size] = product
            started.add((w is ga, t))

        def activate(t):
            lane = lax.broadcasted_iota(jnp.int32, (64, 128), 1)

            @pl.loop(0, 8)
            def _(b):
                rows = pl.ds(pl.multiple_of(b * 64, 64), 64)
                i, to = lax.div(b, 4), pl.ds(pl.multiple_of(lax.rem(b, 4) * 64, 64), 64)
                for k in range(4):
                    at = 128 * k
                    g = acca[t, rows, at : at + 128] if at < GA[h] else accb[t, rows, at - GA[h] : at - GA[h] + 128]
                    u = accb[t, rows, at + 512 - GA[h] : at + 640 - GA[h]]
                    hid[t, i, to, at : at + 128] = (g / (1.0 + jnp.exp(-g)) * u).astype(jnp.bfloat16)
                v = accb[t, rows, GB[h] - 128 : GB[h]]
                end = v / (1.0 + jnp.exp(-v)) * pltpu.roll(v, 64, 1)
                hid[t, i, to, 512:640] = jnp.where(lane < 64, end, 0.0).astype(jnp.bfloat16)

        parts = {
            0: [(m, "land")] + [(m, "b1", i) for i in range(1, 8)],
            1: [(m, "h1w", 1)] + [(m, "h2", i) for i in (0, 2, 4, 6)],
            2: [(m, "h1w", -1)] + [(m, "h2", i) for i in (1, 3, 5, 7)],
            3: [(m, "h2w", 0)],
        }
        blocks = list(dict.fromkeys(at for key, at in arrivals.items() if key[0] == m))
        for t in (0, 1):
            if n == 1:
                before = [(n, "norm", t)] + [(n, g, t, p) for g in ("g2", "g3") for p in (0, 1)]
                cuts = [(s, before, parts[s], 0.62, 0.5) for s in range(4)]
            else:
                whole = [(1, "act", t), (n, "norm", t)] + sum(parts.values(), [])
                cuts = [(p, [(n, g, t, p) for g in ("g2", "g3")] + whole, [], 1.25, 0.7) for p in (0, 1)]
            for s, needs, ready, time_b, time_a in cuts:
                plan.add(
                    (n, "gub", t, s), work=lambda t=t, s=s: dot(accb, gb, t, s), time=time_b, after=needs + ready
                )
                plan.add(
                    (n, "gua", t, s), work=lambda t=t, s=s: dot(acca, ga, t, s), time=time_a, after=needs + blocks
                )
            plan.add(
                (n, "act", t), work=lambda t=t: activate(t), time=0.75,
                after=[(n, k, t, cut[0]) for k in ("gua", "gub") for cut in cuts],
            )

    def scatter(n, m, da, db, add):
        h = n - 1

        def spread(i):
            s, k = origin(i)
            o = zs[-s * k]
            lane = lax.broadcasted_iota(jnp.int32, (16, 128), 1)
            for p in range(NY):
                packed = db[o, p, 64:DROWS].astype(jnp.float32)
                for g in range(4):
                    tile = packed[:, 128 * (g // 2) : 128 * (g // 2) + 128]
                    tile = pltpu.roll(tile, 64, 1) if g % 2 else tile
                    at = 64 * p + 16 * g
                    ends[i, at : at + 16] = jnp.where(lane < 64, tile, 0.0).astype(jnp.bfloat16)

        def product(t, which, i):
            s, k = origin(i)
            o = zs[-s * k]

            def dot(at, size, w):
                return lax.dot_general(
                    hid[t, which, :, at : at + size], w, (((1,), (1,)), ((), ())), preferred_element_type=jnp.float32
                )

            one, two = da[o].reshape(256, 256), db[o, :, 0:64].reshape(256, 256)
            return dot(0, 256, one) + dot(256, 256, two) + dot(512, 128, ends[i])

        def give(t, j):
            for b in range(NB):
                sb[h, J * t + j, b] = product(t, oc, NB * j + b).astype(jnp.bfloat16).reshape(NX, 64, 256)

        def hold(t, j):
            for b in range(NB):
                keep[J * t + j, b] = product(t, c, NB * j + b).reshape(NX, 64, 256)

        def chip(q, b, k, rows):
            return keep[q, b, xs[k], rows] + rb[h, q, b, xs[k], rows].astype(jnp.float32)

        every, low, high = slice(0, 64), slice(0, 32), slice(32, 64)

        def far(q):
            for b in range(NB):
                u1[h, q, 0, b] = chip(q, b, 2, low).astype(jnp.bfloat16)
                u1[h, q, 1, b] = chip(q, b, 2, high).astype(jnp.bfloat16)

        def near(q, d):
            e, some, rest = (0, low, high) if d == 1 else (1, high, low)
            for b in range(NB):
                both = chip(q, b, d, some) + r1[h, q, e, b].astype(jnp.float32)
                u2[h, q, e, b, some] = both.astype(jnp.bfloat16)
                u2[h, q, e, b, rest] = chip(q, b, d, rest).astype(jnp.bfloat16)

        def last(t, j):
            q = J * t + j
            for b in range(NB):
                s, k = origin(NB * j + b)
                cols = pl.ds(pl.multiple_of(zs[-s * k] * 256, 256), 256)
                total = chip(q, b, 0, every)
                total += r2[h, q, 0, b].astype(jnp.float32) + r2[h, q, 1, b].astype(jnp.float32)
                add(slice(64 * t, 64 * t + 64), cols, total)

        for i in range(8):
            needs = block_needs(m, i) + ([] if n == 1 else [(1, "s0k", t, j) for t in (0, 1) for j in range(J)])
            plan.add((m, "spread", i), work=lambda i=i: spread(i), time=0.06, after=needs)
        for t in (0, 1):
            for j in range(J):
                p, q = (t, j), J * t + j
                needs = [(n, "act", t)] + [(m, "spread", i) for i in range(NB * j, NB * j + NB)]
                plan.add(
                    (n, "s0", *p), work=lambda p=p: give(*p), time=0.16 * NB, after=needs,
                    send=[((n, "r0", *p), sb.at[h, q], rb.at[h, q], sib, "c")],
                )
                plan.add((n, "s0k", *p), work=lambda p=p: hold(*p), time=0.16 * NB, after=[(n, "s0", *p)])
                plan.add(
                    (n, "s1", *p), recv=[([(n, "r0", *p)], rb.at[h, q], sib)], after=[(n, "s0k", *p)],
                    work=lambda q=q: far(q), time=0.08,
                    send=[
                        ((n, "r1", d, *p), u1.at[h, q, e], r1.at[h, q, e], xdev[d], f"x{d}")
                        for e, d in ((0, 1), (1, -1))
                    ],
                )
                for e, d in ((0, 1), (1, -1)):
                    plan.add(
                        (n, "s2", d, *p), recv=[([(n, "r1", d, *p)], r1.at[h, q, e], xdev[-d])],
                        after=[(n, "s1", *p)], work=lambda q=q, d=d: near(q, d), time=0.07,
                        send=[((n, "r2", d, *p), u2.at[h, q, e], r2.at[h, q, e], xdev[d], f"x{d}")],
                    )
                plan.add(
                    (n, "s3", *p),
                    recv=[([(n, "r2", d, *p) for d in (1, -1)], r2.at[h, q], xdev[1])],
                    after=[(n, "s1", *p)], work=lambda p=p: last(*p), time=0.15,
                )

    def to_middle(rows, cols, total):
        mid[rows, cols] = (xown[rows, cols].astype(jnp.float32) + 0.5 * total).astype(jnp.bfloat16)

    def to_result(rows, cols, total):
        out[rows, cols] = (mid[rows, cols].astype(jnp.float32) + 0.5 * total).astype(jnp.bfloat16)
        pltpu.make_async_copy(out.at[rows, cols], out_hbm.at[rows, cols], local_sems.at[len(fetches)]).start()

    gather(1, xown, gain1, xn1)
    hidden(1, 1, xn1, ga1, gb1)
    scatter(1, 2, da1, db1, to_middle)
    gather(2, mid, gain2, xn2)
    hidden(2, 3, xn2, ga2, gb2)
    scatter(2, 4, da2, db2, to_result)

    for name in plan.order():
        recv, work, time, send, after = plan.tasks[name]
        with jax.named_scope("_".join(str(p) for p in name)):
            for keys, ref, device in recv:
                net.recv(keys, ref, device)
            if work is not None:
                work()
            for key, src, dst, device, link in send:
                net.send(key, src, dst, device, link)
    net.finish()
    pltpu.make_async_copy(out, out_hbm, local_sems.at[len(fetches)]).wait()


def layer(*args):
    bf, f32 = jnp.bfloat16, jnp.float32
    hbm = pl.BlockSpec(memory_space=pl.ANY)
    chunk = (2 * J, NB)
    return pl.pallas_call(
        kernel,
        out_shape=jax.ShapeDtypeStruct((ROWS, D), bf),
        in_specs=[hbm] * 9,
        out_specs=hbm,
        scratch_shapes=[
            pltpu.VMEM((1, D), f32),
            pltpu.VMEM((1, D), f32),
            pltpu.VMEM((2, 2, 64, H), bf),
            pltpu.VMEM((2, 64, H), bf),
            pltpu.VMEM((ROWS, D), bf),
            pltpu.VMEM((ROWS, D), bf),
            pltpu.VMEM((ROWS, D), bf),
            pltpu.VMEM((NY, NZ, 64, GA[0]), bf),
            pltpu.VMEM((NY, NZ, 64, GB[0]), bf),
            pltpu.VMEM((NY, NZ, 64, GA[1]), bf),
            pltpu.VMEM((NY, NZ, 64, GB[1]), bf),
            pltpu.VMEM((NZ, NY, 64, 256), bf),
            pltpu.VMEM((NZ, NY, DROWS, 256), bf),
            pltpu.VMEM((NZ, NY, 64, 256), bf),
            pltpu.VMEM((NZ, NY, DROWS, 256), bf),
            pltpu.VMEM((2, 2, NX, 64, D), bf),
            pltpu.VMEM((2, 2, NX, 64, D), bf),
            pltpu.VMEM((2, 4 * ROWS, max(GA)), f32),
            pltpu.VMEM((2, 4 * ROWS, max(GB)), f32),
            pltpu.VMEM((2, 2, 2 * ROWS, DK), bf),
            pltpu.VMEM((8, 256, 128), bf),
            pltpu.VMEM((*chunk, NX, 64, 256), f32),
            pltpu.VMEM((2, *chunk, NX, 64, 256), bf),
            pltpu.VMEM((2, *chunk, NX, 64, 256), bf),
            pltpu.VMEM((2, 2 * J, 2, NB, 32, 256), bf),
            pltpu.VMEM((2, 2 * J, 2, NB, 64, 256), bf),
            pltpu.VMEM((2, 2 * J, 2, NB, 32, 256), bf),
            pltpu.VMEM((2, 2 * J, 2, NB, 64, 256), bf),
            pltpu.SemaphoreType.DMA((20,)),
            pltpu.SemaphoreType.DMA((RING * len(LINKS),)),
            pltpu.SemaphoreType.DMA((SEMS,)),
        ],
        compiler_params=pltpu.CompilerParams(
            collective_id=0, has_side_effects=True, vmem_limit_bytes=60 * 2**20
        ),
    )(*args)


def on_device(tokens, norm_one, gate_one, up_one, down_one, norm_two, gate_two, up_two, down_two):
    return layer(
        tokens, gate_one, up_one, down_one.T, gate_two, up_two, down_two.T,
        norm_one.reshape(1, D), norm_two.reshape(1, D),
    )


def solution(mesh):
    return jax.shard_map(
        on_device,
        mesh=mesh,
        in_specs=(
            P(("fs", "tp"), None),
            P(),
            P("fs", "tp"),
            P("fs", "tp"),
            P("tp", "fs"),
            P(),
            P("fs", "tp"),
            P("fs", "tp"),
            P("tp", "fs"),
        ),
        out_specs=P(("fs", "tp"), None),
        check_vma=False,
    )
```
